512 devices in a mesh: sp: 32 (over z, x), tp: 16 (over y, core).
Axes of the slice: x: 4, y: 8, z: 8, core: 2. Of those that a mesh axis runs over, the one named last changes fastest.
Arguments:
- moe_input: bfloat16 [4096, 2048], P('sp'), may hold values from -6 to 6
- out_grad: bfloat16 [4096, 2048], P('sp'), may hold values from -6 to 6
- routes: int32 [4096, 2], P('sp'), may hold values from 0 to 31, all different within a row; in each aligned block of 128 rows (0 to 127, 128 to 255, ...) at most 10 rows name the same one
- route_weight: float32 [4096, 2], P('sp'), may hold values from 0.2 to 1.2
- w_gate: bfloat16 [32, 2048, 2048], P('sp', None, 'tp'), may hold values from -0.125 to 0.125
- w_up: bfloat16 [32, 2048, 2048], P('sp', None, 'tp'), may hold values from -0.125 to 0.125
- w_down: bfloat16 [32, 2048, 2048], P('sp', 'tp'), may hold values from -0.125 to 0.125
- w_out: bfloat16 [2048, 4096], P(None, 'tp'), may hold values from -0.09375 to 0.09375
- query_heads: bfloat16 [16, 4096, 128], P('tp', 'sp'), may hold values from -6 to 6
- key_heads: bfloat16 [16, 4096, 128], P('tp', 'sp'), may hold values from -6 to 6
- value_heads: bfloat16 [16, 4096, 256], P('tp', 'sp'), may hold values from -6 to 6
- log_decay: float32 [16, 4096], P('tp', 'sp'), may hold values from -0.6 to 0
- state_in: float32 [16, 32, 128, 256], P('tp', 'sp'), may hold values from -4 to 4
Outputs:
- gate_grad: bfloat16 [32, 2048, 2048], P('sp', None, 'tp')
- up_grad: bfloat16 [32, 2048, 2048], P('sp', None, 'tp')
- down_grad: bfloat16 [32, 2048, 2048], P('sp', 'tp')
- out_proj_grad: float32 [2048, 4096], P('sp', 'tp')
- query_gradient: bfloat16 [16, 4096, 128], P('tp', 'sp')
- key_grad: bfloat16 [16, 4096, 128], P('tp', 'sp')
- value_grad: bfloat16 [16, 4096, 256], P('tp', 'sp')
The draws below stay inside these ranges and needn't reach their ends.
Inputs may be any that keep to these rules, and one draw needn't show every extreme that they name: `routes`: each row names 2 different experts; within each aligned block of 128 tokens no expert is named more than 10 times, and exactly 10 times for some expert in some blocks.
All inputs are finite; a program needn't handle non-finite values.
Results may differ from the reference program's by a relative error of at most 0.025.
Values may be sent and summed in bfloat16 or wider, within the bound.
A program may use at most 64 MiB of HBM per device.

```python
import math
import jax
import jax.numpy as jnp
import numpy as np
from jax import lax

D = 2048
FF = 2048
RETENTION_HEADS = 16
DK = 128
DV = 256
TOPK = 2
BLOCK = 64
TOK_DEV = 128
SEQUENCE_TOKENS = 4096
EXPERTS = 32
CAP = 10
N_SP = 32
N_TP = 16


def draw_log_decay(key, part):
    random_subkeys = jax.random.split(jax.random.fold_in(key, 11), 6)
    fast_share = 0.5
    quick_heads = jax.random.uniform(random_subkeys[0], (RETENTION_HEADS,), jnp.float32) < fast_share
    fast_rate = jnp.log(10.0) / jax.random.uniform(random_subkeys[1], (RETENTION_HEADS,), jnp.float32, 30.0, 50.0)
    slow_rate = jax.random.uniform(random_subkeys[2], (RETENTION_HEADS,), jnp.float32, 0.2, 0.5) / SEQUENCE_TOKENS
    head_decay_rate = jnp.where(quick_heads, fast_rate, slow_rate)
    span_total = SEQUENCE_TOKENS // TOK_DEV
    span_factor = jnp.exp(jax.random.uniform(random_subkeys[3], (span_total,), jnp.float32, jnp.log(0.5), jnp.log(2.0)))
    position_weighting = jnp.repeat(span_factor, TOK_DEV)
    surge_locations = jax.random.randint(random_subkeys[4], (RETENTION_HEADS, 2), 0, SEQUENCE_TOKENS)
    surge_depth = jnp.log(jax.random.uniform(random_subkeys[5], (RETENTION_HEADS, 2), jnp.float32, 0.6, 0.8))
    token_positions = jnp.arange(SEQUENCE_TOKENS, dtype=jnp.int32)
    match_flags = token_positions[None, :, None] == surge_locations[:, None, :]
    surge_events = jnp.sum(jnp.where(match_flags, surge_depth[:, None, :], 0.0), axis=2)
    logarithm_values = -head_decay_rate[:, None] * position_weighting[None, :] + jnp.where(quick_heads[:, None], 0.0, surge_events)
    return logarithm_values.astype(jnp.float32)


def spiked(values, own_key, source, target, parts, factor):
    owner, partner = [(jnp.arange(values.shape[position]) // (values.shape[position] // parts)).reshape([-1 if axis == position else 1 for axis in range(values.ndim)]) for position in (source, target)]
    chosen = jax.random.permutation(own_key, parts)[partner]
    strong = (owner == chosen) | (owner == (partner + parts // 2) % parts)
    return jnp.where(strong, factor * values, values)


def block_scale(own_key, shape, shards, least, top_value):
    def one(position, blocks):
        heights = jax.random.uniform(jax.random.fold_in(jax.random.fold_in(own_key, 6), position), (blocks,), jnp.float32, least / len(shards), top_value / len(shards))
        return jnp.repeat(jnp.exp(heights), shape[position] // blocks).reshape((-1,) + (1,) * (len(shape) - position - 1))

    loudness = one(*shards[0])
    for cut in shards[1:]:
        loudness = loudness * one(*cut)
    return loudness


def deal_out(rng, own, number, rows, number_of, top, reach, slope):
    ranking = jax.random.permutation(rng, number_of)
    heavy_load, ordinary = load_shares(number_of, rows * top, reach, slope, True), load_shares(number_of, rows * top, reach, slope, False)
    places = jnp.arange(number_of)

    def named(sizes, offset_by):
        used = int((sizes > 0).sum())
        fixed = max(1, used // 4)
        moved = fixed + (places - fixed + offset_by * (used - fixed)) % max(1, number_of - fixed)
        return jnp.zeros((number_of,), jnp.int32).at[ranking[jnp.where(places < fixed, places, moved)]].set(jnp.asarray(sizes, jnp.int32))

    sizes = jnp.where(number % 4 == 0, named(heavy_load, number // 4), named(ordinary, number - number // 4 - 1))
    mixed = jax.random.permutation(jax.random.fold_in(own, 3), number_of)
    giver, taker = mixed[0:number_of // 2 * 2:2], mixed[1:number_of // 2 * 2:2]
    room = jnp.minimum(sizes[giver] - 1, reach - sizes[taker]) // 2
    room = jnp.where((giver == ranking[0]) | (taker == ranking[0]) | (sizes[taker] == 0), 0, jnp.maximum(room, 0))
    moved = jax.random.randint(jax.random.fold_in(own, 4), (number_of // 2,), 0, 1 << 20) % (room + 1)
    sizes = sizes.at[giver].add(-moved).at[taker].add(moved)
    items = jnp.searchsorted(jnp.cumsum(sizes), jnp.arange(rows * top), side="right").astype(jnp.int32)
    grid = items.reshape(top, rows).T
    grid = grid[jax.random.permutation(jax.random.fold_in(own, 1), rows)]
    offset_by = jax.random.randint(jax.random.fold_in(own, 2), (rows, 1), 0, top)
    return jnp.take_along_axis(grid, (jnp.arange(top)[None, :] + offset_by) % top, axis=1)


def load_shares(amount, total, most, lean, full):
    weights = [(1 << 20) // math.isqrt(rank ** lean) + 1 for rank in range(1, amount + 1)]
    largest = most if full else min(most, max(-(-total // amount), total * weights[0] // sum(weights)))
    least = 1 if total - largest >= amount - 1 else 0
    counts, rest = [largest] + [least] * (amount - 1), total - largest - least * (amount - 1)
    while rest > 0:
        free = [i for i in range(1, amount) if counts[i] < largest] or [i for i in range(1, amount) if counts[i] < most]
        whole, remaining = sum([weights[i] for i in free]), rest
        for i in free:
            extra = min(most - counts[i], max(1, remaining * weights[i] // whole), rest)
            counts[i] = counts[i] + extra
            rest = rest - extra
    return np.array(counts)


def bell_draw(own_key, shape, width, reach, shards=(), kind=jnp.bfloat16):
    entries = width * jax.random.normal(own_key, shape, jnp.float32)
    if shards:
        entries = entries * block_scale(own_key, shape, shards, -0.22, 0.18)
    return jnp.clip(entries, -reach, reach).astype(kind)


def bell_draw_with(stream_key, dims, scale, most, shards, heavy, kind=jnp.bfloat16):
    values = scale * jax.random.normal(stream_key, dims, jnp.float32)
    if shards:
        values = values * block_scale(stream_key, dims, shards, -0.22, 0.18)
    return jnp.clip(spiked(values, jax.random.fold_in(stream_key, 3), *heavy), -most, most).astype(kind)


def setup_inputs(seed: int = 0) -> dict:
    streams_of = jax.random.split(jax.random.key(seed), 14)
    moe_input = bell_draw(streams_of[0], (SEQUENCE_TOKENS, D), 1.0, 6.0, ((0, 32),))
    out_grad = bell_draw_with(streams_of[1], (SEQUENCE_TOKENS, D), 1.0, 6.0, ((0, 32),), (0, 1, 32, 2.75))
    routes_keys = jax.random.split(jax.random.fold_in(streams_of[2], 1), SEQUENCE_TOKENS // TOK_DEV)
    routes_turns = jax.random.permutation(jax.random.fold_in(streams_of[2], 3), SEQUENCE_TOKENS // TOK_DEV)
    routes = jax.vmap(lambda own, number: deal_out(jax.random.fold_in(streams_of[2], 2), own, number, TOK_DEV, EXPERTS, TOPK, CAP, 2))(routes_keys, routes_turns).reshape((SEQUENCE_TOKENS, TOPK))
    route_weight = jnp.clip(0.2 + 1 * jax.random.uniform(streams_of[3], (SEQUENCE_TOKENS, TOPK), jnp.float32) ** block_scale(streams_of[3], (SEQUENCE_TOKENS, TOPK), ((0, 32),), -0.2, 0.2), 0.2, 1.2)
    w_gate = bell_draw(streams_of[4], (EXPERTS, D, FF), D ** -0.5, 0.125, ((0, 32), (2, 16)))
    w_up = bell_draw(streams_of[5], (EXPERTS, D, FF), D ** -0.5, 0.125, ((0, 32), (2, 16)))
    w_down = bell_draw(streams_of[6], (EXPERTS, FF, D), FF ** -0.5, 0.125, ((0, 32), (1, 16)))
    w_out = bell_draw(streams_of[7], (D, RETENTION_HEADS * DV), (RETENTION_HEADS * DV) ** -0.5, 0.09375, ((1, 16),))
    query_heads = bell_draw(streams_of[8], (RETENTION_HEADS, SEQUENCE_TOKENS, DK), 1.0, 6.0, ((0, 16), (1, 32)))
    key_heads = bell_draw(streams_of[9], (RETENTION_HEADS, SEQUENCE_TOKENS, DK), 1.0, 6.0, ((0, 16), (1, 32)))
    value_heads = bell_draw(streams_of[10], (RETENTION_HEADS, SEQUENCE_TOKENS, DV), 1.0, 6.0, ((0, 16), (1, 32)))
    log_decay = draw_log_decay(jax.random.fold_in(streams_of[13], 71), 0)
    state_in = bell_draw(streams_of[12], (RETENTION_HEADS, N_SP, DK, DV), 0.5, 4.0, ((0, 16), (1, 32)), jnp.float32)
    return dict(moe_input=moe_input, out_grad=out_grad, routes=routes, route_weight=route_weight, w_gate=w_gate, w_up=w_up, w_down=w_down, w_out=w_out, query_heads=query_heads, key_heads=key_heads, value_heads=value_heads, log_decay=log_decay, state_in=state_in)


exact_precision = lax.Precision.HIGHEST


def stored(array):
    return lax.optimization_barrier(array.astype(jnp.bfloat16))


def silu_slope(gate_pre):
    sigmoid_v = jax.nn.sigmoid(gate_pre)
    return sigmoid_v * (1.0 + gate_pre * (1.0 - sigmoid_v))


def decay_table(log_sums):
    block_size = log_sums.shape[-1]
    token_positions = jnp.arange(block_size)
    lower_mask = (token_positions[:, None] >= token_positions[None, :])[None]
    log_diff = jnp.where(lower_mask, log_sums[:, :, None] - log_sums[:, None, :], 0.0)
    return jnp.where(lower_mask, jnp.exp(log_diff), 0.0)


def forward_block(forwarded_state, inputs):
    query_rows, rescaled_keys, value_rows, head_gradients, log_sums = inputs
    decay_mat = decay_table(log_sums)
    scores = jnp.einsum('htk,hsk->hts', query_rows, rescaled_keys, precision=exact_precision) * decay_mat
    leading_decay = jnp.exp(log_sums)[:, :, None]
    trailing_decay = jnp.exp(log_sums[:, -1:] - log_sums)[:, :, None]
    blended_heads = jnp.einsum('hts,hsv->htv', scores, value_rows, precision=exact_precision)
    blended_heads = blended_heads + jnp.einsum('imj,iju->imu', query_rows * leading_decay, forwarded_state, precision=exact_precision)
    back_scores = jnp.einsum('htv,hsv->hts', head_gradients, value_rows, precision=exact_precision) * decay_mat
    query_gradient = jnp.einsum('hts,hsk->htk', back_scores, rescaled_keys, precision=exact_precision)
    query_gradient = query_gradient + jnp.einsum('fqg,fug->fqu', head_gradients * leading_decay, forwarded_state, precision=exact_precision)
    forwarded_state = jnp.exp(log_sums[:, -1])[:, None, None] * forwarded_state + jnp.einsum(
        'nbq,nbc->nqc', rescaled_keys * trailing_decay, value_rows, precision=exact_precision)
    return forwarded_state, (blended_heads, query_gradient)


def reverse_block(forwarded_state, inputs):
    query_rows, rescaled_keys, value_rows, head_gradients, log_sums = inputs
    decay_mat = decay_table(log_sums)
    scores = jnp.einsum('htk,hsk->hts', query_rows, rescaled_keys, precision=exact_precision) * decay_mat
    back_scores = jnp.einsum('htv,hsv->hts', head_gradients, value_rows, precision=exact_precision) * decay_mat
    leading_decay = jnp.exp(log_sums)[:, :, None]
    trailing_decay = jnp.exp(log_sums[:, -1:] - log_sums)[:, :, None]
    key_portion = jnp.einsum('hts,htk->hsk', back_scores, query_rows, precision=exact_precision)
    key_portion = key_portion + jnp.einsum('lbg,ljg->lbj', value_rows * trailing_decay, forwarded_state, precision=exact_precision)
    value_portion = jnp.einsum('hts,htv->hsv', scores, head_gradients, precision=exact_precision)
    value_portion = value_portion + jnp.einsum('bea,baz->bez', rescaled_keys * trailing_decay, forwarded_state, precision=exact_precision)
    forwarded_state = jnp.exp(log_sums[:, -1])[:, None, None] * forwarded_state + jnp.einsum(
        'byj,byg->bjg', query_rows * leading_decay, head_gradients, precision=exact_precision)
    return forwarded_state, (key_portion, value_portion)


def reference(moe_input, out_grad, routes, route_weight, w_gate, w_up, w_down, w_out,
              query_heads, key_heads, value_heads, log_decay, state_in):
    routed_all = TOK_DEV * TOPK
    route_ids = routes.reshape(N_SP, routed_all)
    onehot = (route_ids[:, :, None] == jnp.arange(EXPERTS, dtype=jnp.int32)[None, None, :]).astype(jnp.int32)
    slot_index = jnp.sum(jnp.cumsum(onehot, axis=1) * onehot, axis=2) - 1
    anchor = jnp.arange(N_SP, dtype=jnp.int32)[:, None]
    row_place = (anchor * CAP + slot_index).astype(jnp.int32)
    token_id = (anchor * TOK_DEV + jnp.arange(routed_all, dtype=jnp.int32)[None, :] // TOPK).astype(jnp.int32)
    expert_rows = N_SP * CAP
    token_table = jnp.full((EXPERTS, expert_rows), -1, jnp.int32).at[route_ids, row_place].set(token_id)
    weight_table = jnp.zeros((EXPERTS, expert_rows), jnp.float32).at[route_ids, row_place].set(
        route_weight.reshape(N_SP, routed_all))
    group_width = FF // N_TP

    def one_expert(expert_items):
        token_row, weight_row, gate_w, up_w, down_w = expert_items
        filled = token_row >= 0
        picked = jnp.where(filled, token_row, 0)
        rows_in = jnp.where(filled[:, None], moe_input[picked], jnp.zeros((), jnp.bfloat16))
        scaled = stored(jnp.where(filled[:, None], weight_row[:, None] * out_grad[picked].astype(jnp.float32), 0.0))
        gate_pre = jnp.dot(rows_in, gate_w, preferred_element_type=jnp.float32)
        up_pre = jnp.dot(rows_in, up_w, preferred_element_type=jnp.float32)
        active = jax.nn.silu(gate_pre)
        hidden = stored(active * up_pre)
        hidden_back = jnp.dot(scaled, down_w.T, preferred_element_type=jnp.float32)
        down_part = jnp.dot(hidden.T, scaled, preferred_element_type=jnp.float32).astype(jnp.bfloat16)
        gate_back = stored(hidden_back * up_pre * silu_slope(gate_pre))
        up_back = stored(hidden_back * active)
        gate_part = jnp.dot(rows_in.T, gate_back, preferred_element_type=jnp.float32).astype(jnp.bfloat16)
        up_part = jnp.dot(rows_in.T, up_back, preferred_element_type=jnp.float32).astype(jnp.bfloat16)
        groups_gate = gate_back.astype(jnp.float32).reshape(expert_rows, N_TP, group_width)
        groups_up = up_back.astype(jnp.float32).reshape(expert_rows, N_TP, group_width)
        weights_gate = gate_w.astype(jnp.float32).reshape(D, N_TP, group_width)
        weights_up = up_w.astype(jnp.float32).reshape(D, N_TP, group_width)
        partial_value = jnp.einsum('rgf,dgf->grd', groups_gate, weights_gate)
        partial_value = partial_value + jnp.einsum('rgf,dgf->grd', groups_up, weights_up)
        route_back = jnp.sum(stored(partial_value).astype(jnp.float32), axis=0).astype(jnp.bfloat16)
        return gate_part, up_part, down_part, route_back

    gate_grad, up_grad, down_grad, route_back = lax.map(
        one_expert, (token_table, weight_table, w_gate, w_up, w_down))
    returned = route_back[route_ids, row_place].reshape(SEQUENCE_TOKENS, TOPK, D)
    mixed_grad = (out_grad.astype(jnp.float32) + jnp.sum(returned.astype(jnp.float32), axis=1)).astype(jnp.bfloat16)

    head_grad = stored(jnp.dot(mixed_grad, w_out, preferred_element_type=jnp.float32))
    head_gradients = head_grad.astype(jnp.float32).reshape(SEQUENCE_TOKENS, RETENTION_HEADS, DV).transpose(1, 0, 2)
    block_count = SEQUENCE_TOKENS // BLOCK
    per_span = TOK_DEV // BLOCK

    def to_blocks(array):
        return array.reshape(RETENTION_HEADS, block_count, BLOCK, array.shape[-1]).transpose(1, 0, 2, 3)

    def from_blocks(array):
        return array.transpose(1, 0, 2, 3).reshape(RETENTION_HEADS, SEQUENCE_TOKENS, array.shape[-1])

    query_rows = query_heads.astype(jnp.float32)
    rescaled_keys = key_heads.astype(jnp.float32) * DK ** -0.5
    value_rows = value_heads.astype(jnp.float32)
    log_sums = jnp.cumsum(log_decay.reshape(RETENTION_HEADS, block_count, BLOCK), axis=2).transpose(1, 0, 2)
    inputs = (to_blocks(query_rows), to_blocks(rescaled_keys), to_blocks(value_rows), to_blocks(head_gradients), log_sums)

    def forward_step(forwarded_state, block_items):
        block_index = block_items[-1]
        fresh_state = lax.dynamic_index_in_dim(state_in, block_index // per_span, axis=1, keepdims=False)
        start_state = jnp.where(block_index % per_span == 0, fresh_state, forwarded_state)
        return forward_block(start_state, block_items[:-1])

    empty_state = jnp.zeros((RETENTION_HEADS, DK, DV), jnp.float32)
    _, (blended_heads, query_gradient) = lax.scan(
        forward_step, empty_state, inputs + (jnp.arange(block_count, dtype=jnp.int32),))
    _, (key_grad, value_grad) = lax.scan(reverse_block, empty_state, inputs, reverse=True)
    mixed_flat = from_blocks(blended_heads).astype(jnp.bfloat16).transpose(1, 0, 2).reshape(SEQUENCE_TOKENS, RETENTION_HEADS * DV)
    out_proj_grad = jnp.dot(mixed_grad.T, mixed_flat, preferred_element_type=jnp.float32)
    query_gradient = from_blocks(query_gradient).astype(jnp.bfloat16)
    key_grad = (from_blocks(key_grad) * DK ** -0.5).astype(jnp.bfloat16)
    value_grad = from_blocks(value_grad).astype(jnp.bfloat16)
    return gate_grad, up_grad, down_grad, out_proj_grad, query_gradient, key_grad, value_grad
```

```python
import functools

import jax
import jax.numpy as jnp
from jax import lax
from jax.experimental import pallas as pl
from jax.experimental.pallas import tpu as pltpu
from jax.sharding import Mesh
from jax.sharding import PartitionSpec as P

BLOCK = 64
SP = ("sp_0", "sp_1")
BF = jnp.bfloat16
F32 = jnp.float32
MSG = 16


def mm(a, b, dims=((1,), (0,))):
    return lax.dot_general(a, b, (dims, ((), ())), preferred_element_type=F32)


def silu_slope_of(v, sig):
    return sig * (1.0 + v * (1.0 - sig))


def front_kernel(
    sizes,
    x_hbm, g_hbm, routes_ref, rw_ref, wg_hbm, wu_hbm, wd_hbm,
    gg_ref, ug_ref, dg_ref, mix_ref,
    xs, gs, wgu, wd, pt, send, recv, rows, acc_gu, acc_hb, gbub, hid,
    part, part_in, out_r, out_l, in_r, in_l, back, ret, mixed,
    load_sem, a2a_send, a2a_recv, ag_send, ag_recv, pp_send, pp_recv,
    rs_send, rs_recv, ret_send, ret_recv, mg_send, mg_recv,
):
    n_sp, n_tp, cap, slots = sizes
    n_chip = n_tp // 2
    half = n_chip // 2
    tok = x_hbm.shape[0]
    width = xs.shape[1]
    n_rows = n_sp * cap
    hr = n_rows // 2
    s, t = lax.axis_index("sp"), lax.axis_index("tp")
    chip, par = t // 2, t % 2
    partner = t + 1 - 2 * par

    def tp_of(c, parity=None):
        return lax.rem(c + 2 * n_chip, n_chip) * 2 + (par if parity is None else parity)

    right, left = tp_of(chip + 1), tp_of(chip - 1)

    def remote(src, dst, ssem, rsem, where):
        return pltpu.make_async_remote_copy(
            src_ref=src, dst_ref=dst, send_sem=ssem, recv_sem=rsem,
            device_id=where, device_id_type=pl.DeviceIdType.MESH,
        )

    share = pl.ds(pl.multiple_of(t * width, width), width)
    loads = [
        pltpu.make_async_copy(x_hbm.at[:, share], xs, load_sem.at[0]),
        pltpu.make_async_copy(g_hbm.at[:, share], gs, load_sem.at[1]),
        pltpu.make_async_copy(wg_hbm, wgu.at[:, pl.ds(0, width)], load_sem.at[2]),
        pltpu.make_async_copy(wu_hbm, wgu.at[:, pl.ds(width, width)], load_sem.at[3]),
        pltpu.make_async_copy(wd_hbm, wd, load_sem.at[4]),
    ]
    for c in loads:
        c.start()

    recv[...] = jnp.zeros_like(recv)
    ret[...] = jnp.zeros_like(ret)
    barrier = pltpu.get_barrier_semaphore()

    def greet_sp(d, carry):
        pl.semaphore_signal(
            barrier, inc=1, device_id={"sp": lax.rem(s + d, n_sp), "tp": t},
            device_id_type=pl.DeviceIdType.MESH)
        return carry

    def greet_tp(d, carry):
        pl.semaphore_signal(
            barrier, inc=1, device_id={"sp": s, "tp": tp_of(chip + d)},
            device_id_type=pl.DeviceIdType.MESH)
        return carry

    lax.fori_loop(1, n_sp, greet_sp, 0)
    lax.fori_loop(1, n_chip, greet_tp, 0)
    pl.semaphore_signal(barrier, inc=1, device_id={"sp": s, "tp": partner},
                        device_id_type=pl.DeviceIdType.MESH)

    r0, r1 = routes_ref[:, 0:1], routes_ref[:, 1:2]
    lane = lax.broadcasted_iota(jnp.int32, (tok, n_sp * slots), 1)
    expert, place = lane // slots, lane % slots
    first, second = r0 == expert, r1 == expert
    named = jnp.where(first | second, 1.0, 0.0)
    row_i = lax.broadcasted_iota(jnp.int32, (tok, tok), 0)
    col_i = lax.broadcasted_iota(jnp.int32, (tok, tok), 1)
    earlier = jnp.where(col_i < row_i, 1.0, 0.0).astype(BF)
    count = mm(earlier, named.astype(BF))
    here = count == place.astype(F32)
    p0 = jnp.where(first & here, 1.0, 0.0).astype(BF)
    p1 = jnp.where(second & here, 1.0, 0.0).astype(BF)
    pt[...] = jnp.where((first | second) & here, 1.0, 0.0).astype(BF)
    loads[0].wait()
    loads[1].wait()
    gf = gs[...].astype(F32)
    sg0 = (rw_ref[:, 0:1] * gf).astype(BF)
    sg1 = (rw_ref[:, 1:2] * gf).astype(BF)
    xv = xs[...]
    sendrows = mm(p0, jnp.concatenate([xv, sg0], axis=1), ((0,), (0,)))
    sendrows += mm(p1, jnp.concatenate([xv, sg1], axis=1), ((0,), (0,)))
    send[...] = sendrows.astype(BF)

    pl.semaphore_wait(barrier, n_sp - 1 + n_chip - 1 + 1)

    def block(ref, e, length=slots):
        return ref.at[pl.ds(pl.multiple_of(e * slots, slots), length)]

    def dispatch(d, carry):
        e = lax.rem(s + d, n_sp)
        remote(block(send, e, MSG), block(recv, s, MSG), a2a_send.at[e], a2a_recv.at[s],
               {"sp": e, "tp": t}).start()
        return carry

    lax.fori_loop(1, n_sp, dispatch, 0)
    recv[pl.ds(pl.multiple_of(s * slots, slots), slots), :] = send[
        pl.ds(pl.multiple_of(s * slots, slots), slots), :]

    def arrived(d, carry):
        e = lax.rem(s + d, n_sp)
        c = remote(block(send, e, MSG), block(recv, e, MSG), a2a_send.at[e], a2a_recv.at[e],
                   {"sp": e, "tp": t})
        c.wait()
        return carry

    lax.fori_loop(1, n_sp, arrived, 0)

    dense_r = lax.broadcasted_iota(jnp.int32, (n_rows, n_sp * slots), 0)
    padded_c = lax.broadcasted_iota(jnp.int32, (n_rows, n_sp * slots), 1)
    squeeze = jnp.where(
        padded_c == (dense_r // cap) * slots + dense_r % cap, 1.0, 0.0).astype(BF)
    packed = mm(squeeze, recv[...]).astype(BF)
    rows[t, 0] = packed[:, :width]
    rows[t, 1] = packed[:, width:]

    started = []

    def pass_on(origin, u, where, k):
        c = remote(rows.at[origin, u], rows.at[origin, u], ag_send.at[k], ag_recv.at[origin, u],
                   {"sp": s, "tp": where})
        c.start()
        started.append(c)

    def await_rows(origin, u):
        remote(rows.at[origin, u], rows.at[origin, u], ag_send.at[0], ag_recv.at[origin, u],
               {"sp": s, "tp": partner}).wait_recv()

    n_sent = 0

    def next_sem():
        nonlocal n_sent
        n_sent += 1
        return n_sent - 1

    def goes(direction, u, k):
        return k < half or (k == half and u == direction)

    for u in (0, 1):
        if goes(0, u, 1):
            pass_on(t, u, right, next_sem())
        if goes(1, u, 1):
            pass_on(t, u, left, next_sem())
    for u in (0, 1):
        pass_on(t, u, partner, next_sem())

    acc_gu[...] = jnp.zeros_like(acc_gu)
    acc_hb[...] = jnp.zeros_like(acc_hb)
    for c in loads[2:]:
        c.wait()

    def feats(c):
        return pl.ds(pl.multiple_of(c * 2 * width, 2 * width), 2 * width)

    def forward(c):
        for u in (0, 1):
            await_rows(tp_of(c, 1 - par), u)
        xin = jnp.concatenate([rows[2 * c, 0], rows[2 * c + 1, 0]], axis=1)
        gin = jnp.concatenate([rows[2 * c, 1], rows[2 * c + 1, 1]], axis=1)
        acc_gu[...] += mm(xin, wgu[feats(c), :])
        acc_hb[...] += mm(gin, wd[:, feats(c)], ((1,), (1,)))

    ready = [chip]
    for k in range(1, half + 1):
        from_left, from_right = lax.rem(chip - k + n_chip, n_chip), lax.rem(chip + k, n_chip)
        for u in (0, 1):
            if goes(0, u, k):
                o = from_left * 2 + par
                await_rows(o, u)
                if goes(0, u, k + 1):
                    pass_on(o, u, right, next_sem())
                pass_on(o, u, partner, next_sem())
            if goes(1, u, k):
                o = from_right * 2 + par
                await_rows(o, u)
                if goes(1, u, k + 1):
                    pass_on(o, u, left, next_sem())
                pass_on(o, u, partner, next_sem())
        for c in ready:
            forward(c)
        ready = [from_left, from_right] if k < half else [from_left]
    for c in ready:
        forward(c)
    for c in started:
        c.wait_send()

    gate_pre, up_pre = acc_gu[:, :width], acc_gu[:, width:]
    sig = jax.nn.sigmoid(gate_pre)
    active = gate_pre * sig
    hb = acc_hb[...]
    hid[...] = (active * up_pre).astype(BF)
    gbub[:, :width] = (hb * up_pre * silu_slope_of(gate_pre, sig)).astype(BF)
    gbub[:, width:] = (hb * active).astype(BF)

    order = [chip + half]
    for k in range(half - 1, 0, -1):
        order += [chip + k, chip - k]
    order = [lax.rem(c + n_chip, n_chip) for c in order + [chip]]
    shared = []
    gb_all = gbub[...]
    for n, c in enumerate(order):
        value = mm(gb_all, wgu[feats(c), :], ((1,), (1,))).astype(BF)
        part[c, 0] = value[:, :width]
        part[c, 1] = value[:, width:]
        cp = remote(part.at[c, 1 - par], part_in.at[c], pp_send.at[n], pp_recv.at[c],
                    {"sp": s, "tp": partner})
        cp.start()
        shared.append(cp)

    def await_part(c):
        remote(part.at[c, 1 - par], part_in.at[c], pp_send.at[0], pp_recv.at[c],
               {"sp": s, "tp": partner}).wait_recv()

    cut = (pl.ds(0, hr), pl.ds(hr, hr))
    sums = []

    def ring_copy(direction, i, h):
        out, inn = (out_r, in_r) if direction == 0 else (out_l, in_l)
        return remote(out.at[i - 1, cut[h]], inn.at[i - 1, cut[h]],
                      rs_send.at[direction, i - 1, h], rs_recv.at[direction, i - 1, h],
                      {"sp": s, "tp": right if direction == 0 else left})

    def has(direction, i, h):
        return i >= 2 or h == direction

    for i in range(1, half + 1):
        d = half + 1 - i
        targets = (lax.rem(chip + d, n_chip), lax.rem(chip - d + n_chip, n_chip))
        if i == 1:
            await_part(targets[0])
        else:
            await_part(targets[0])
            await_part(targets[1])
        for h in (0, 1):
            for direction in (0, 1):
                if not has(direction, i, h):
                    continue
                out, inn = (out_r, in_r) if direction == 0 else (out_l, in_l)
                c = targets[direction]
                total = part[c, par, cut[h], :].astype(F32) + part_in[c, cut[h], :].astype(F32)
                if i >= 2 and has(direction, i - 1, h):
                    ring_copy(direction, i - 1, h).wait_recv()
                    total += inn[i - 2, cut[h], :].astype(F32)
                out[i - 1, cut[h], :] = total.astype(BF)
                cp = ring_copy(direction, i, h)
                cp.start()
                sums.append(cp)
    await_part(chip)
    pieces = []
    for h in (0, 1):
        total = part[chip, par, cut[h], :].astype(F32) + part_in[chip, cut[h], :].astype(F32)
        for direction in (0, 1):
            if has(direction, half, h):
                ring_copy(direction, half, h).wait_recv()
                inn = in_r if direction == 0 else in_l
                total += inn[half - 1, cut[h], :].astype(F32)
        pieces.append(total.astype(BF))
    summed = jnp.concatenate(pieces, axis=0)

    padded_r = lax.broadcasted_iota(jnp.int32, (n_sp * slots, n_rows), 0)
    dense_c = lax.broadcasted_iota(jnp.int32, (n_sp * slots, n_rows), 1)
    spread = jnp.where(
        padded_r == (dense_c // cap) * slots + dense_c % cap, 1.0, 0.0).astype(BF)
    back[...] = mm(spread, summed).astype(BF)

    def send_back(d, carry):
        e = lax.rem(s + d, n_sp)
        remote(block(back, e, MSG), block(ret, s, MSG), ret_send.at[e], ret_recv.at[s],
               {"sp": e, "tp": t}).start()
        return carry

    lax.fori_loop(1, n_sp, send_back, 0)
    ret[pl.ds(pl.multiple_of(s * slots, slots), slots), :] = back[
        pl.ds(pl.multiple_of(s * slots, slots), slots), :]

    hid_all = hid[...]
    for c in range(n_chip):
        xin = jnp.concatenate([rows[2 * c, 0], rows[2 * c + 1, 0]], axis=1)
        gin = jnp.concatenate([rows[2 * c, 1], rows[2 * c + 1, 1]], axis=1)
        both = mm(xin, gb_all, ((0,), (0,)))
        at = pl.ds(c * 2 * width, 2 * width)
        gg_ref[at, :] = both[:, :width].astype(BF)
        ug_ref[at, :] = both[:, width:].astype(BF)
        dg_ref[:, at] = mm(hid_all, gin, ((0,), (0,))).astype(BF)
    for cp in shared + sums:
        cp.wait_send()

    def returned(d, carry):
        e = lax.rem(s + d, n_sp)
        remote(block(back, e, MSG), block(ret, e, MSG), ret_send.at[e], ret_recv.at[e],
               {"sp": e, "tp": t}).wait()
        return carry

    lax.fori_loop(1, n_sp, returned, 0)
    mixed[t] = (gs[...].astype(F32) + mm(pt[...], ret[...])).astype(BF)

    def mixed_copy(origin, where, k):
        return remote(mixed.at[origin], mixed.at[origin], mg_send.at[k], mg_recv.at[origin],
                      {"sp": s, "tp": where})

    copies = []
    for d in range(half, 0, -1):
        for c in sorted({d, n_chip - d}):
            cp = mixed_copy(t, tp_of(chip + c), c)
            cp.start()
            copies.append(cp)
    cp = mixed_copy(t, partner, 0)
    cp.start()
    copies.append(cp)
    for d in range(1, half + 1):
        for c in sorted({d, n_chip - d}):
            o = tp_of(chip + c)
            mixed_copy(o, partner, n_chip + c).wait_recv()
            cp = mixed_copy(o, partner, n_chip + c)
            cp.start()
            copies.append(cp)
    for d in range(n_chip):
        mixed_copy(tp_of(chip + d, 1 - par), partner, 0).wait_recv()
    for o in range(n_tp):
        mix_ref[:, o * width:(o + 1) * width] = mixed[o]
    for cp in copies:
        cp.wait_send()


def front(n_sp, n_tp, moe_input, out_grad, routes, route_weight, w_gate, w_up, w_down):
    tok, model = moe_input.shape
    cap = 5 * tok * routes.shape[1] // (4 * n_sp)
    slots = -(-cap // 16) * 16
    width = model // n_tp
    hidden = w_gate.shape[1]
    n_rows = n_sp * cap
    n_chip = n_tp // 2
    half = n_chip // 2
    hbm = pl.BlockSpec(memory_space=pl.ANY)
    vmem = pl.BlockSpec(memory_space=pltpu.VMEM)
    dma = pltpu.SemaphoreType.DMA
    n_ag = 2 * (2 * half - 1) + 2 * n_chip
    return pl.pallas_call(
        functools.partial(front_kernel, (n_sp, n_tp, cap, slots)),
        name="front",
        out_shape=(
            jax.ShapeDtypeStruct((model, hidden), BF),
            jax.ShapeDtypeStruct((model, hidden), BF),
            jax.ShapeDtypeStruct((hidden, model), BF),
            jax.ShapeDtypeStruct((tok, model), BF),
        ),
        in_specs=[hbm, hbm, vmem, vmem, hbm, hbm, hbm],
        out_specs=(vmem, vmem, vmem, vmem),
        scratch_shapes=[
            pltpu.VMEM((tok, width), BF),
            pltpu.VMEM((tok, width), BF),
            pltpu.VMEM((model, 2 * hidden), BF),
            pltpu.VMEM((hidden, model), BF),
            pltpu.VMEM((tok, n_sp * slots), BF),
            pltpu.VMEM((n_sp * slots, 2 * width), BF),
            pltpu.VMEM((n_sp * slots, 2 * width), BF),
            pltpu.VMEM((n_tp, 2, n_rows, width), BF),
            pltpu.VMEM((n_rows, 2 * hidden), F32),
            pltpu.VMEM((n_rows, hidden), F32),
            pltpu.VMEM((n_rows, 2 * hidden), BF),
            pltpu.VMEM((n_rows, hidden), BF),
            pltpu.VMEM((n_chip, 2, n_rows, width), BF),
            pltpu.VMEM((n_chip, n_rows, width), BF),
            pltpu.VMEM((half, n_rows, width), BF),
            pltpu.VMEM((half, n_rows, width), BF),
            pltpu.VMEM((half, n_rows, width), BF),
            pltpu.VMEM((half, n_rows, width), BF),
            pltpu.VMEM((n_sp * slots, width), BF),
            pltpu.VMEM((n_sp * slots, width), BF),
            pltpu.VMEM((n_tp, tok, width), BF),
            dma((5,)),
            dma((n_sp,)),
            dma((n_sp,)),
            dma((n_ag,)),
            dma((n_tp, 2)),
            dma((n_chip,)),
            dma((n_chip,)),
            dma((2, half, 2)),
            dma((2, half, 2)),
            dma((n_sp,)),
            dma((n_sp,)),
            dma((2 * n_chip,)),
            dma((n_tp,)),
        ],
        compiler_params=pltpu.CompilerParams(
            collective_id=0, has_side_effects=True, vmem_limit_bytes=48 << 20
        ),
    )(moe_input, out_grad, routes, route_weight, w_gate, w_up, w_down)


def neutral_like(shard, identity):
    return jax.tree.map(
        lambda a, e: jnp.broadcast_to(jnp.asarray(e, a.dtype), a.shape), shard, identity
    )


def prefix_by_axis(shard, axes, combine, identity):
    before = start = neutral_like(shard, identity)
    subtotal = shard
    for axis in reversed(axes):
        length, position = (lax.axis_size(axis), lax.axis_index(axis))
        pieces = jax.tree.map(
            lambda part, kind: lax.all_gather(part.astype(kind), axis),
            subtotal,
            (jnp.bfloat16, jnp.bfloat16),
        )
        inside, subtotal = (start, start)
        for k in reversed(range(length)):
            passed = k > position
            subtotal = combine(
                subtotal, jax.tree.map(lambda part, own: part[k].astype(own.dtype), pieces, shard)
            )
            inside = jax.tree.map(lambda new, old: jnp.where(passed, new, old), subtotal, inside)
        before = combine(inside, before)
    return before


def cut_along(shard, dim, length):
    lengths = shard.shape
    pieces = shard.reshape(*lengths[:dim], length, lengths[dim] // length, *lengths[dim + 1 :])
    return jnp.moveaxis(pieces, dim, 0)


def summed_on_arrival(shard, axis, dim):
    pieces = cut_along(shard, dim, lax.axis_size(axis))
    arrived = lax.all_to_all(pieces, axis, split_axis=0, concat_axis=0, tiled=True)
    return arrived.astype(jnp.float32).sum(axis=0)


def silu_slope(gate_pre):
    sigmoid_v = jax.nn.sigmoid(gate_pre)
    return sigmoid_v * (1.0 + gate_pre * (1.0 - sigmoid_v))


def decay_table(log_sums):
    block_size = log_sums.shape[-1]
    token_positions = jnp.arange(block_size)
    lower_mask = (token_positions[:, None] >= token_positions[None, :])[None]
    log_diff = jnp.where(lower_mask, log_sums[:, :, None] - log_sums[:, None, :], 0.0)
    return jnp.where(lower_mask, jnp.exp(log_diff), 0.0)


def forward_block(forwarded_state, inputs):
    query_rows, rescaled_keys, value_rows, head_gradients, log_sums = inputs
    decay_mat = decay_table(log_sums)
    scores = jnp.einsum("htk,hsk->hts", query_rows, rescaled_keys) * decay_mat
    leading_decay = jnp.exp(log_sums)[:, :, None]
    trailing_decay = jnp.exp(log_sums[:, -1:] - log_sums)[:, :, None]
    blended_heads = jnp.einsum("hts,hsv->htv", scores, value_rows)
    blended_heads = blended_heads + jnp.einsum(
        "imj,iju->imu", query_rows * leading_decay, forwarded_state
    )
    back_scores = jnp.einsum("htv,hsv->hts", head_gradients, value_rows) * decay_mat
    query_gradient = jnp.einsum("hts,hsk->htk", back_scores, rescaled_keys)
    query_gradient = query_gradient + jnp.einsum(
        "fqg,fug->fqu", head_gradients * leading_decay, forwarded_state
    )
    forwarded_state = jnp.exp(log_sums[:, -1])[:, None, None] * forwarded_state + jnp.einsum(
        "nbq,nbc->nqc", rescaled_keys * trailing_decay, value_rows
    )
    return (forwarded_state, (blended_heads, query_gradient))


def reverse_block(forwarded_state, inputs):
    query_rows, rescaled_keys, value_rows, head_gradients, log_sums = inputs
    decay_mat = decay_table(log_sums)
    scores = jnp.einsum("htk,hsk->hts", query_rows, rescaled_keys) * decay_mat
    back_scores = jnp.einsum("htv,hsv->hts", head_gradients, value_rows) * decay_mat
    leading_decay = jnp.exp(log_sums)[:, :, None]
    trailing_decay = jnp.exp(log_sums[:, -1:] - log_sums)[:, :, None]
    key_portion = jnp.einsum("hts,htk->hsk", back_scores, query_rows)
    key_portion = key_portion + jnp.einsum(
        "lbg,ljg->lbj", value_rows * trailing_decay, forwarded_state
    )
    value_portion = jnp.einsum("hts,htv->hsv", scores, head_gradients)
    value_portion = value_portion + jnp.einsum(
        "bea,baz->bez", rescaled_keys * trailing_decay, forwarded_state
    )
    forwarded_state = jnp.exp(log_sums[:, -1])[:, None, None] * forwarded_state + jnp.einsum(
        "byj,byg->bjg", query_rows * leading_decay, head_gradients
    )
    return (forwarded_state, (key_portion, value_portion))


def link_states(higher_part, lower_part):
    return (
        higher_part[0] * lower_part[0],
        lower_part[1] + lower_part[0][:, None, None] * higher_part[1],
    )


def tail(mixed_grad, w_out, query_heads, key_heads, value_heads, log_decay, state_in):
    tok_rows = mixed_grad.shape[0]
    head_count = query_heads.shape[0]
    key_size = key_heads.shape[-1]
    value_size = value_heads.shape[-1]
    head_grad = jnp.dot(mixed_grad, w_out, preferred_element_type=jnp.float32).astype(jnp.bfloat16)
    head_gradients = (
        head_grad.reshape(tok_rows, head_count, value_size).transpose(1, 0, 2).astype(jnp.float32)
    )
    query_rows = query_heads.astype(jnp.float32)
    rescaled_keys = key_heads.astype(jnp.float32) * key_size ** (-0.5)
    value_rows = value_heads.astype(jnp.float32)
    block_count = tok_rows // BLOCK

    def to_blocks(array):
        return array.reshape(head_count, block_count, BLOCK, array.shape[-1]).transpose(1, 0, 2, 3)

    def from_blocks(array):
        return array.transpose(1, 0, 2, 3).reshape(head_count, tok_rows, array.shape[-1])

    log_sums = jnp.cumsum(log_decay.reshape(head_count, block_count, BLOCK), axis=2).transpose(
        1, 0, 2
    )
    inputs = (
        to_blocks(query_rows),
        to_blocks(rescaled_keys),
        to_blocks(value_rows),
        to_blocks(head_gradients),
        log_sums,
    )
    _, (blended_heads, query_gradient) = lax.scan(forward_block, state_in[:, 0], inputs)
    running_total = jnp.cumsum(log_decay, axis=1)
    carried = jnp.einsum(
        "byj,byg->bjg", query_rows * jnp.exp(running_total)[:, :, None], head_gradients
    )
    span_keep = jnp.exp(running_total[:, -1])
    incoming = prefix_by_axis(
        (span_keep, carried), SP, link_states, (jnp.ones_like(span_keep), jnp.zeros_like(carried))
    )[1]
    _, (key_grad, value_grad) = lax.scan(reverse_block, incoming, inputs, reverse=True)
    mixed_flat = (
        from_blocks(blended_heads)
        .astype(jnp.bfloat16)
        .transpose(1, 0, 2)
        .reshape(tok_rows, head_count * value_size)
    )
    out_proj_grad = summed_on_arrival(
        lax.dot_general(
            mixed_grad, mixed_flat, (((0,), (0,)), ((), ())), preferred_element_type=jnp.float32
        ).astype(jnp.bfloat16),
        SP,
        0,
    )
    query_gradient = from_blocks(query_gradient).astype(jnp.bfloat16)
    key_grad = (from_blocks(key_grad) * key_size ** (-0.5)).astype(jnp.bfloat16)
    value_grad = from_blocks(value_grad).astype(jnp.bfloat16)
    return (out_proj_grad, query_gradient, key_grad, value_grad)


def solution(mesh):
    n_sp, n_tp = mesh.shape["sp"], mesh.shape["tp"]
    finer = Mesh(mesh.devices.reshape(8, 4, n_tp), ("sp_0", "sp_1", "tp"))

    def first(moe_input, out_grad, routes, route_weight, w_gate, w_up, w_down):
        gate_grad, up_grad, down_grad, mixed = front(
            n_sp, n_tp, moe_input, out_grad, routes, route_weight, w_gate[0], w_up[0], w_down[0]
        )
        return gate_grad[None], up_grad[None], down_grad[None], mixed

    first = jax.shard_map(
        first,
        mesh=mesh,
        in_specs=(
            P("sp", None),
            P("sp", None),
            P("sp", None),
            P("sp", None),
            P("sp", None, "tp"),
            P("sp", None, "tp"),
            P("sp", "tp", None),
        ),
        out_specs=(P("sp", None, "tp"), P("sp", None, "tp"), P("sp", "tp", None), P("sp", None)),
        check_vma=False,
    )
    second = jax.shard_map(
        tail,
        mesh=finer,
        in_specs=(
            P(SP, None),
            P(None, "tp"),
            P("tp", SP, None),
            P("tp", SP, None),
            P("tp", SP, None),
            P("tp", SP),
            P("tp", SP, None, None),
        ),
        out_specs=(P(SP, "tp"), P("tp", SP, None), P("tp", SP, None), P("tp", SP, None)),
        check_vma=False,
    )

    def whole(
        moe_input, out_grad, routes, route_weight, w_gate, w_up, w_down, w_out,
        query_heads, key_heads, value_heads, log_decay, state_in,
    ):
        *grads, mixed = first(moe_input, out_grad, routes, route_weight, w_gate, w_up, w_down)
        rest = second(mixed, w_out, query_heads, key_heads, value_heads, log_decay, state_in)
        return (*grads, *rest)

    return whole
```

```python
import functools

import jax
import jax.numpy as jnp
from jax import lax
from jax.experimental import pallas as pl
from jax.experimental.pallas import tpu as pltpu
from jax.sharding import PartitionSpec as P

X_CHIPS = 4
BF = jnp.bfloat16
F32 = jnp.float32
MSG = 16


def mm(a, b, dims=((1,), (0,))):
    return lax.dot_general(a, b, (dims, ((), ())), preferred_element_type=F32)


def silu_slope_of(v, sig):
    return sig * (1.0 + v * (1.0 - sig))


def kernel(
    sizes,
    x_hbm, g_hbm, routes_ref, rw_ref, wg_hbm, wu_hbm, wd_hbm,
    wo_hbm, q_hbm, k_hbm, v_hbm, decay_ref, state_hbm,
    gg_ref, ug_ref, dg_ref, og_ref, qg_ref, kg_ref, vg_ref,
    xs, gs, wgu, wd, pt, send, recv, rows, acc_gu, acc_hb, gbub, hid,
    part, part_in, out_r, out_l, in_r, in_l, back, ret, mixed,
    wo, qv, kv, vv, st, heads, keep_out, keep_in, carried, pieces_in, pieces_out, s_in,
    mg_out, mg_in, scores_v, acc_hg,
    load_sem, a2a_send, a2a_recv, ag_send, ag_recv, pp_send, pp_recv,
    rs_send, rs_recv, ret_send, ret_recv, mg_send, mg_recv,
    keep_send, keep_recv, hx_send, hx_recv, hz_send, hz_recv,
    sc_send, sc_recv, sb_send, sb_recv, op_send, op_recv,
):
    n_sp, n_tp, n_x, cap, slots = sizes
    n_z = n_sp // n_x
    z_half = n_z // 2
    n_chip = n_tp // 2
    half = n_chip // 2
    tok = x_hbm.shape[0]
    width = xs.shape[1]
    n_rows = n_sp * cap
    hr = n_rows // 2
    s, t = lax.axis_index("sp"), lax.axis_index("tp")
    chip, par = t // 2, t % 2
    partner = t + 1 - 2 * par

    def tp_of(c, parity=None):
        return lax.rem(c + 2 * n_chip, n_chip) * 2 + (par if parity is None else parity)

    right, left = tp_of(chip + 1), tp_of(chip - 1)
    z, x = s // n_x, s % n_x

    def sp_of(zz, xx):
        return lax.rem(zz + n_z, n_z) * n_x + lax.rem(xx + n_x, n_x)

    def remote(src, dst, ssem, rsem, where):
        return pltpu.make_async_remote_copy(
            src_ref=src, dst_ref=dst, send_sem=ssem, recv_sem=rsem,
            device_id=where, device_id_type=pl.DeviceIdType.MESH,
        )

    share = pl.ds(pl.multiple_of(t * width, width), width)
    loads = [
        pltpu.make_async_copy(x_hbm.at[:, share], xs, load_sem.at[0]),
        pltpu.make_async_copy(g_hbm.at[:, share], gs, load_sem.at[1]),
        pltpu.make_async_copy(wg_hbm, wgu.at[:, pl.ds(0, width)], load_sem.at[2]),
        pltpu.make_async_copy(wu_hbm, wgu.at[:, pl.ds(width, width)], load_sem.at[3]),
        pltpu.make_async_copy(wd_hbm, wd, load_sem.at[4]),
        pltpu.make_async_copy(q_hbm, qv, load_sem.at[5]),
        pltpu.make_async_copy(k_hbm, kv, load_sem.at[6]),
        pltpu.make_async_copy(v_hbm, vv, load_sem.at[7]),
        pltpu.make_async_copy(state_hbm, st, load_sem.at[8]),
        pltpu.make_async_copy(wo_hbm, wo, load_sem.at[9]),
    ]
    for c in loads:
        c.start()

    recv[...] = jnp.zeros_like(recv)
    ret[...] = jnp.zeros_like(ret)
    barrier = pltpu.get_barrier_semaphore()

    def greet_sp(d, carry):
        pl.semaphore_signal(
            barrier, inc=1, device_id={"sp": lax.rem(s + d, n_sp), "tp": t},
            device_id_type=pl.DeviceIdType.MESH)
        return carry

    def greet_tp(d, carry):
        pl.semaphore_signal(
            barrier, inc=1, device_id={"sp": s, "tp": tp_of(chip + d)},
            device_id_type=pl.DeviceIdType.MESH)
        return carry

    lax.fori_loop(1, n_sp, greet_sp, 0)
    lax.fori_loop(1, n_chip, greet_tp, 0)
    pl.semaphore_signal(barrier, inc=1, device_id={"sp": s, "tp": partner},
                        device_id_type=pl.DeviceIdType.MESH)

    r0, r1 = routes_ref[0:1, :], routes_ref[1:2, :]
    line = lax.broadcasted_iota(jnp.int32, (n_sp * slots, tok), 0)
    expert, place = line // slots, line % slots
    first, second = r0 == expert, r1 == expert
    named = jnp.where(first | second, 1.0, 0.0)
    row_i = lax.broadcasted_iota(jnp.int32, (tok, tok), 0)
    col_i = lax.broadcasted_iota(jnp.int32, (tok, tok), 1)
    earlier = jnp.where(row_i < col_i, 1.0, 0.0).astype(BF)
    count = mm(named.astype(BF), earlier)
    here = count == place.astype(F32)
    p0 = jnp.where(first & here, 1.0, 0.0).astype(BF)
    p1 = jnp.where(second & here, 1.0, 0.0).astype(BF)
    pt[...] = jnp.where((first | second) & here, 1.0, 0.0).astype(BF)

    def column(row):
        return jnp.sum(jnp.where(row_i == col_i, row, 0.0), axis=1, keepdims=True)

    loads[0].wait()
    loads[1].wait()
    gf = gs[...].astype(F32)
    sg0 = (column(rw_ref[0:1, :]) * gf).astype(BF)
    sg1 = (column(rw_ref[1:2, :]) * gf).astype(BF)
    xv = xs[...]
    sendrows = mm(p0, jnp.concatenate([xv, sg0], axis=1))
    sendrows += mm(p1, jnp.concatenate([xv, sg1], axis=1))
    send[...] = sendrows.astype(BF)

    pl.semaphore_wait(barrier, n_sp - 1 + n_chip - 1 + 1)

    def block(ref, e, length=slots):
        return ref.at[pl.ds(pl.multiple_of(e * slots, slots), length)]

    def dispatch(d, carry):
        e = lax.rem(s + d, n_sp)
        remote(block(send, e, MSG), block(recv, s, MSG), a2a_send.at[e], a2a_recv.at[s],
               {"sp": e, "tp": t}).start()
        return carry

    lax.fori_loop(1, n_sp, dispatch, 0)
    recv[pl.ds(pl.multiple_of(s * slots, slots), slots), :] = send[
        pl.ds(pl.multiple_of(s * slots, slots), slots), :]

    for c in loads[5:9]:
        c.wait()
    decay_col = column(decay_ref[...])
    upto = jnp.where(col_i <= row_i, decay_ref[...], 0.0)
    sum_col = jnp.sum(upto, axis=1, keepdims=True)
    sum_row = jnp.sum(jnp.where(row_i <= col_i, decay_col, 0.0), axis=0, keepdims=True)
    end = jnp.sum(decay_ref[...], axis=1, keepdims=True)
    lower = col_i <= row_i
    table = jnp.where(lower, jnp.exp(jnp.where(lower, sum_col - sum_row, 0.0)), 0.0)
    lead, trail = jnp.exp(sum_col), jnp.exp(end - sum_col)
    keep_out[...] = jnp.broadcast_to(jnp.exp(end), keep_out.shape)
    scale = qv.shape[1] ** -0.5
    q_all, k_all, v_all = qv[...], kv[...], vv[...]
    q_lead = (q_all.astype(F32) * lead).astype(BF)
    scores = (mm(q_all, k_all, ((1,), (1,))) * scale * table).astype(BF)
    scores_v[...] = scores
    state = st[...].astype(BF)
    made = (mm(scores, v_all) + mm(q_lead, state)).astype(BF)
    ht = tok // 2
    mine = pl.ds(pl.multiple_of(s * ht, ht), ht)
    heads[0, mine, :] = made[:ht]
    heads[1, mine, :] = made[ht:]

    def arrived(d, carry):
        e = lax.rem(s + d, n_sp)
        c = remote(block(send, e, MSG), block(recv, e, MSG), a2a_send.at[e], a2a_recv.at[e],
                   {"sp": e, "tp": t})
        c.wait()
        return carry

    lax.fori_loop(1, n_sp, arrived, 0)

    def give_keep(d, carry):
        e = lax.rem(s + d, n_sp)
        remote(keep_out, keep_in.at[s], keep_send.at[e], keep_recv.at[s],
               {"sp": e, "tp": t}).start()
        return carry

    head_copies = []

    def across(h, owner, where, k):
        at = pl.ds(pl.multiple_of(owner * ht, ht), ht)
        return remote(heads.at[h, at], heads.at[h, at], hx_send.at[h, k],
                      hx_recv.at[h, owner % n_x], {"sp": where, "tp": t})

    def along(h, row, where, k):
        at = pl.ds(pl.multiple_of(row * n_x * ht, n_x * ht), n_x * ht)
        return remote(heads.at[h, at], heads.at[h, at], hz_send.at[k], hz_recv.at[h, row],
                      {"sp": where, "tp": t})

    def z_goes(direction, h, k):
        return k < z_half or (k == z_half and h == direction)

    z_sent = [0]

    def z_send(h, row, direction):
        c = along(h, row, sp_of(z + 1 if direction == 0 else z - 1, x), z_sent[0])
        z_sent[0] += 1
        c.start()
        head_copies.append(c)

    def heads_step(k):
        for h in (0, 1):
            if k == 0:
                for d in range(1, n_x):
                    across(h, sp_of(z, x + d), s, d - 1).wait_recv()
                for direction in (0, 1):
                    if z_goes(direction, h, 1):
                        z_send(h, z, direction)
                continue
            for direction in (0, 1):
                if not z_goes(direction, h, k):
                    continue
                row = lax.rem(z - k + n_z if direction == 0 else z + k, n_z)
                along(h, row, s, 0).wait_recv()
                if z_goes(direction, h, k + 1):
                    z_send(h, row, direction)

    dense_r = lax.broadcasted_iota(jnp.int32, (n_rows, n_sp * slots), 0)
    padded_c = lax.broadcasted_iota(jnp.int32, (n_rows, n_sp * slots), 1)
    squeeze = jnp.where(
        padded_c == (dense_r // cap) * slots + dense_r % cap, 1.0, 0.0).astype(BF)
    packed = mm(squeeze, recv[...]).astype(BF)
    rows[t, 0] = packed[:, :width]
    rows[t, 1] = packed[:, width:]

    started = []

    def pass_on(origin, u, where, k):
        c = remote(rows.at[origin, u], rows.at[origin, u], ag_send.at[k], ag_recv.at[origin, u],
                   {"sp": s, "tp": where})
        c.start()
        started.append(c)

    def await_rows(origin, u):
        remote(rows.at[origin, u], rows.at[origin, u], ag_send.at[0], ag_recv.at[origin, u],
               {"sp": s, "tp": partner}).wait_recv()

    n_sent = 0

    def next_sem():
        nonlocal n_sent
        n_sent += 1
        return n_sent - 1

    def goes(direction, u, k):
        return k < half or (k == half and u == direction)

    for u in (0, 1):
        if goes(0, u, 1):
            pass_on(t, u, right, next_sem())
        if goes(1, u, 1):
            pass_on(t, u, left, next_sem())
    for u in (0, 1):
        pass_on(t, u, partner, next_sem())

    for h in (0, 1):
        for d in range(1, n_x):
            c = across(h, s, sp_of(z, x + d), d - 1)
            c.start()
            head_copies.append(c)
    keep_in[s] = keep_out[...]
    lax.fori_loop(1, n_sp, give_keep, 0)
    acc_gu[...] = jnp.zeros_like(acc_gu)
    acc_hb[...] = jnp.zeros_like(acc_hb)
    for c in loads[2:5]:
        c.wait()

    def feats(c):
        return pl.ds(pl.multiple_of(c * 2 * width, 2 * width), 2 * width)

    def forward(c):
        for u in (0, 1):
            await_rows(tp_of(c, 1 - par), u)
        xin = jnp.concatenate([rows[2 * c, 0], rows[2 * c + 1, 0]], axis=1)
        gin = jnp.concatenate([rows[2 * c, 1], rows[2 * c + 1, 1]], axis=1)
        acc_gu[...] += mm(xin, wgu[feats(c), :])
        acc_hb[...] += mm(gin, wd[:, feats(c)], ((1,), (1,)))

    ready = [chip]
    for k in range(1, half + 1):
        from_left, from_right = lax.rem(chip - k + n_chip, n_chip), lax.rem(chip + k, n_chip)
        for u in (0, 1):
            if goes(0, u, k):
                o = from_left * 2 + par
                await_rows(o, u)
                if goes(0, u, k + 1):
                    pass_on(o, u, right, next_sem())
                pass_on(o, u, partner, next_sem())
            if goes(1, u, k):
                o = from_right * 2 + par
                await_rows(o, u)
                if goes(1, u, k + 1):
                    pass_on(o, u, left, next_sem())
                pass_on(o, u, partner, next_sem())
        for c in ready:
            forward(c)
        if k - 1 <= z_half:
            heads_step(k - 1)
        ready = [from_left, from_right] if k < half else [from_left]
    for c in ready:
        forward(c)
    for c in started:
        c.wait_send()

    gate_pre, up_pre = acc_gu[:, :width], acc_gu[:, width:]
    sig = jax.nn.sigmoid(gate_pre)
    active = gate_pre * sig
    hb = acc_hb[...]
    hid[...] = (active * up_pre).astype(BF)
    gbub[:, :width] = (hb * up_pre * silu_slope_of(gate_pre, sig)).astype(BF)
    gbub[:, width:] = (hb * active).astype(BF)

    order = [chip + half]
    for k in range(half - 1, 0, -1):
        order += [chip + k, chip - k]
    order = [lax.rem(c + n_chip, n_chip) for c in order + [chip]]
    shared = []
    gb_all = gbub[...]
    for n, c in enumerate(order):
        value = mm(gb_all, wgu[feats(c), :], ((1,), (1,))).astype(BF)
        part[c, 0] = value[:, :width]
        part[c, 1] = value[:, width:]
        cp = remote(part.at[c, 1 - par], part_in.at[c], pp_send.at[n], pp_recv.at[c],
                    {"sp": s, "tp": partner})
        cp.start()
        shared.append(cp)

    def await_part(c):
        remote(part.at[c, 1 - par], part_in.at[c], pp_send.at[0], pp_recv.at[c],
               {"sp": s, "tp": partner}).wait_recv()

    cut = (pl.ds(0, hr), pl.ds(hr, hr))
    sums = []

    def ring_copy(direction, i, h):
        out, inn = (out_r, in_r) if direction == 0 else (out_l, in_l)
        return remote(out.at[i - 1, cut[h]], inn.at[i - 1, cut[h]],
                      rs_send.at[direction, i - 1, h], rs_recv.at[direction, i - 1, h],
                      {"sp": s, "tp": right if direction == 0 else left})

    def has(direction, i, h):
        return i >= 2 or h == direction

    for i in range(1, half + 1):
        d = half + 1 - i
        targets = (lax.rem(chip + d, n_chip), lax.rem(chip - d + n_chip, n_chip))
        if i == 1:
            await_part(targets[0])
        else:
            await_part(targets[0])
            await_part(targets[1])
        for h in (0, 1):
            for direction in (0, 1):
                if not has(direction, i, h):
                    continue
                out, inn = (out_r, in_r) if direction == 0 else (out_l, in_l)
                c = targets[direction]
                total = part[c, par, cut[h], :].astype(F32) + part_in[c, cut[h], :].astype(F32)
                if i >= 2 and has(direction, i - 1, h):
                    ring_copy(direction, i - 1, h).wait_recv()
                    total += inn[i - 2, cut[h], :].astype(F32)
                out[i - 1, cut[h], :] = total.astype(BF)
                cp = ring_copy(direction, i, h)
                cp.start()
                sums.append(cp)
    for k in range(half, z_half + 1):
        heads_step(k)
    await_part(chip)
    pieces = []
    for h in (0, 1):
        total = part[chip, par, cut[h], :].astype(F32) + part_in[chip, cut[h], :].astype(F32)
        for direction in (0, 1):
            if has(direction, half, h):
                ring_copy(direction, half, h).wait_recv()
                inn = in_r if direction == 0 else in_l
                total += inn[half - 1, cut[h], :].astype(F32)
        pieces.append(total.astype(BF))
    summed = jnp.concatenate(pieces, axis=0)

    padded_r = lax.broadcasted_iota(jnp.int32, (n_sp * slots, n_rows), 0)
    dense_c = lax.broadcasted_iota(jnp.int32, (n_sp * slots, n_rows), 1)
    spread = jnp.where(
        padded_r == (dense_c // cap) * slots + dense_c % cap, 1.0, 0.0).astype(BF)
    back[...] = mm(spread, summed).astype(BF)

    def send_back(d, carry):
        e = lax.rem(s + d, n_sp)
        remote(block(back, e, MSG), block(ret, s, MSG), ret_send.at[e], ret_recv.at[s],
               {"sp": e, "tp": t}).start()
        return carry

    lax.fori_loop(1, n_sp, send_back, 0)
    ret[pl.ds(pl.multiple_of(s * slots, slots), slots), :] = back[
        pl.ds(pl.multiple_of(s * slots, slots), slots), :]

    hid_all = hid[...]
    for c in range(n_chip):
        xin = jnp.concatenate([rows[2 * c, 0], rows[2 * c + 1, 0]], axis=1)
        gin = jnp.concatenate([rows[2 * c, 1], rows[2 * c + 1, 1]], axis=1)
        both = mm(xin, gb_all, ((0,), (0,)))
        at = pl.ds(c * 2 * width, 2 * width)
        gg_ref[at, :] = both[:, :width].astype(BF)
        ug_ref[at, :] = both[:, width:].astype(BF)
        dg_ref[:, at] = mm(hid_all, gin, ((0,), (0,))).astype(BF)
    for cp in shared + sums:
        cp.wait_send()

    def returned(d, carry):
        e = lax.rem(s + d, n_sp)
        remote(block(back, e, MSG), block(ret, e, MSG), ret_send.at[e], ret_recv.at[e],
               {"sp": e, "tp": t}).wait()
        return carry

    lax.fori_loop(1, n_sp, returned, 0)
    mixed[t] = (gs[...].astype(F32) + mm(pt[...], ret[...], ((0,), (0,)))).astype(BF)

    def mixed_copy(origin, where, k):
        return remote(mixed.at[origin], mixed.at[origin], mg_send.at[k], mg_recv.at[origin],
                      {"sp": s, "tp": where})

    copies = []
    for d in range(half, 0, -1):
        for c in sorted({d, n_chip - d}):
            cp = mixed_copy(t, tp_of(chip + c), c)
            cp.start()
            copies.append(cp)
    cp = mixed_copy(t, partner, 0)
    cp.start()
    copies.append(cp)
    for d in range(1, half + 1):
        for c in sorted({d, n_chip - d}):
            o = tp_of(chip + c)
            mixed_copy(o, partner, n_chip + c).wait_recv()
            cp = mixed_copy(o, partner, n_chip + c)
            cp.start()
            copies.append(cp)
    loads[9].wait()
    acc_hg[...] = jnp.zeros_like(acc_hg)
    for d in range(half + 1):
        for c in sorted({d, (n_chip - d) % n_chip}):
            o = lax.rem(chip + c, n_chip)
            mixed_copy(o * 2 + 1 - par, partner, 0).wait_recv()
            acc_hg[...] += mm(jnp.concatenate([mixed[2 * o], mixed[2 * o + 1]], axis=1), wo[feats(o), :])

    hg = acc_hg[...].astype(BF)
    carried[...] = mm(q_lead, hg, ((0,), (0,)))
    pr = pieces_in.shape[1]

    def piece(ref, i):
        return ref.at[pl.ds(pl.multiple_of((i // 2) * pr, 8), pr),
                      pl.ds(pl.multiple_of((i % 2) * 128, 128), 128)]

    def give_piece(d, carry):
        e = lax.rem(s + d, n_sp)
        remote(piece(carried, e), pieces_in.at[s], sc_send.at[e], sc_recv.at[s],
               {"sp": e, "tp": t}).start()
        return carry

    lax.fori_loop(1, n_sp, give_piece, 0)
    pieces_in[s] = piece(carried, s)[...]
    back_scores = (mm(hg, v_all, ((1,), (1,))) * table).astype(BF)
    hg_lead = (acc_hg[...].astype(BF).astype(F32) * lead).astype(BF)

    lane = lax.broadcasted_iota(jnp.int32, (ht, width), 1)
    for o in range(n_tp):
        both = mixed[o].astype(F32)
        top, bottom = both[:ht], both[ht:]
        mg_out[2 * o] = jnp.where(lane < 64, top, pltpu.roll(bottom, 64, 1)).astype(BF)
        mg_out[2 * o + 1] = jnp.where(lane < 64, pltpu.roll(top, 64, 1), bottom).astype(BF)

    def mg_piece(e):
        return mg_in.at[pl.ds(pl.multiple_of(e * ht, ht), ht)]

    def give_mg(d, carry):
        e = lax.rem(s + d, n_sp)
        remote(mg_out.at[e], mg_piece(s), op_send.at[e], op_recv.at[s], {"sp": e, "tp": t}).start()
        return carry

    lax.fori_loop(1, n_sp, give_mg, 0)
    mg_in[mine, :] = mg_out[s]

    qg_ref[...] = (mm(back_scores, k_all) * scale + mm(hg_lead, state, ((1,), (1,)))).astype(BF)
    key_part = mm(back_scores, q_all, ((0,), (0,)))
    value_part = mm(scores_v[...], hg, ((0,), (0,)))

    def keep_here(d, carry):
        e = lax.rem(s + d, n_sp)
        remote(keep_out, keep_in.at[e], keep_send.at[e], keep_recv.at[e], {"sp": e, "tp": t}).wait()
        return carry

    lax.fori_loop(1, n_sp, keep_here, 0)

    def piece_here(d, carry):
        e = lax.rem(s + d, n_sp)
        remote(piece(carried, e), pieces_in.at[e], sc_send.at[e], sc_recv.at[e],
               {"sp": e, "tp": t}).wait()
        return carry

    lax.fori_loop(1, n_sp, piece_here, 0)
    running = jnp.zeros(pieces_in.shape[1:], F32)
    for p in range(n_sp - 1, -1, -1):
        pieces_out[p] = running
        running = pieces_in[p] + keep_in[p][0:1, :] * running

    def give_state(d, carry):
        e = lax.rem(s + d, n_sp)
        remote(pieces_out.at[e], piece(s_in, s), sb_send.at[e], sb_recv.at[s],
               {"sp": e, "tp": t}).start()
        return carry

    lax.fori_loop(1, n_sp, give_state, 0)
    piece(s_in, s)[...] = pieces_out[s]

    def mg_here(d, carry):
        e = lax.rem(s + d, n_sp)
        remote(mg_out.at[e], mg_piece(e), op_send.at[e], op_recv.at[e], {"sp": e, "tp": t}).wait()
        return carry

    lax.fori_loop(1, n_sp, mg_here, 0)
    slices = mg_in[...]
    og_ref[...] = (mm(slices, heads[0], ((0,), (0,)))[: width // 2]
                   + mm(slices, heads[1], ((0,), (0,)))[width // 2:])

    def state_here(d, carry):
        e = lax.rem(s + d, n_sp)
        remote(pieces_out.at[e], piece(s_in, e), sb_send.at[e], sb_recv.at[e],
               {"sp": e, "tp": t}).wait()
        return carry

    lax.fori_loop(1, n_sp, state_here, 0)
    later = s_in[...].astype(BF)
    v_trail = (v_all.astype(F32) * trail).astype(BF)
    k_trail = (k_all.astype(F32) * (scale * trail)).astype(BF)
    kg_ref[...] = ((key_part + mm(v_trail, later, ((1,), (1,)))) * scale).astype(BF)
    vg_ref[...] = (value_part + mm(k_trail, later)).astype(BF)
    for cp in copies + head_copies:
        cp.wait_send()


def program(sizes, moe_input, out_grad, routes, route_weight, w_gate, w_up, w_down,
            w_out, query, key, value, log_decay, state_in):
    n_sp, n_tp, n_x = sizes
    tok, model = moe_input.shape
    cap = 5 * tok * routes.shape[0] // (4 * n_sp)
    slots = -(-cap // 16) * 16
    width = model // n_tp
    hidden = w_gate.shape[1]
    n_rows = n_sp * cap
    n_chip = n_tp // 2
    half = n_chip // 2
    n_z = n_sp // n_x
    dk, dv = query.shape[1], value.shape[1]
    pr = dk * dv // (128 * n_sp)
    hbm = pl.BlockSpec(memory_space=pltpu.HBM)
    vmem = pl.BlockSpec(memory_space=pltpu.VMEM)
    dma = pltpu.SemaphoreType.DMA
    n_ag = 2 * (2 * half - 1) + 2 * n_chip
    return pl.pallas_call(
        functools.partial(kernel, (n_sp, n_tp, n_x, cap, slots)),
        name="whole",
        out_shape=(
            jax.ShapeDtypeStruct((model, hidden), BF),
            jax.ShapeDtypeStruct((model, hidden), BF),
            jax.ShapeDtypeStruct((hidden, model), BF),
            jax.ShapeDtypeStruct((model // n_sp, dv), F32),
            jax.ShapeDtypeStruct((tok, dk), BF),
            jax.ShapeDtypeStruct((tok, dk), BF),
            jax.ShapeDtypeStruct((tok, dv), BF),
        ),
        in_specs=[hbm, hbm, vmem, vmem, hbm, hbm, hbm, hbm, hbm, hbm, hbm, vmem, hbm],
        out_specs=(vmem,) * 7,
        scratch_shapes=[
            pltpu.VMEM((tok, width), BF),
            pltpu.VMEM((tok, width), BF),
            pltpu.VMEM((model, 2 * hidden), BF),
            pltpu.VMEM((hidden, model), BF),
            pltpu.VMEM((n_sp * slots, tok), BF),
            pltpu.VMEM((n_sp * slots, 2 * width), BF),
            pltpu.VMEM((n_sp * slots, 2 * width), BF),
            pltpu.VMEM((n_tp, 2, n_rows, width), BF),
            pltpu.VMEM((n_rows, 2 * hidden), F32),
            pltpu.VMEM((n_rows, hidden), F32),
            pltpu.VMEM((n_rows, 2 * hidden), BF),
            pltpu.VMEM((n_rows, hidden), BF),
            pltpu.VMEM((n_chip, 2, n_rows, width), BF),
            pltpu.VMEM((n_chip, n_rows, width), BF),
            pltpu.VMEM((half, n_rows, width), BF),
            pltpu.VMEM((half, n_rows, width), BF),
            pltpu.VMEM((half, n_rows, width), BF),
            pltpu.VMEM((half, n_rows, width), BF),
            pltpu.VMEM((n_sp * slots, width), BF),
            pltpu.VMEM((n_sp * slots, width), BF),
            pltpu.VMEM((n_tp, tok, width), BF),
            pltpu.VMEM((model, dv), BF),
            pltpu.VMEM((tok, dk), BF),
            pltpu.VMEM((tok, dk), BF),
            pltpu.VMEM((tok, dv), BF),
            pltpu.VMEM((dk, dv), F32),
            pltpu.VMEM((2, n_sp * tok // 2, dv), BF),
            pltpu.VMEM((8, 128), F32),
            pltpu.VMEM((n_sp, 8, 128), F32),
            pltpu.VMEM((dk, dv), F32),
            pltpu.VMEM((n_sp, pr, 128), F32),
            pltpu.VMEM((n_sp, pr, 128), F32),
            pltpu.VMEM((dk, dv), F32),
            pltpu.VMEM((n_sp, tok // 2, width), BF),
            pltpu.VMEM((n_sp * tok // 2, width), BF),
            pltpu.VMEM((tok, tok), BF),
            pltpu.VMEM((tok, dv), F32),
            dma((10,)),
            dma((n_sp,)),
            dma((n_sp,)),
            dma((n_ag,)),
            dma((n_tp, 2)),
            dma((n_chip + 1,)),
            dma((n_chip,)),
            dma((2, half, 2)),
            dma((2, half, 2)),
            dma((n_sp,)),
            dma((n_sp,)),
            dma((2 * n_chip,)),
            dma((n_tp,)),
            dma((n_sp,)),
            dma((n_sp,)),
            dma((2, n_x)),
            dma((2, n_x)),
            dma((2 * n_z,)),
            dma((2, n_z)),
            dma((n_sp,)),
            dma((n_sp,)),
            dma((n_sp,)),
            dma((n_sp,)),
            dma((n_sp,)),
            dma((n_sp,)),
        ],
        compiler_params=pltpu.CompilerParams(
            collective_id=0, has_side_effects=True, vmem_limit_bytes=60 << 20
        ),
    )(moe_input, out_grad, routes, route_weight, w_gate, w_up, w_down,
      w_out, query, key, value, log_decay, state_in)


def solution(mesh):
    sizes = (mesh.shape["sp"], mesh.shape["tp"], X_CHIPS)

    def body(moe_input, out_grad, routes, route_weight, w_gate, w_up, w_down,
             w_out, query, key, value, log_decay, state_in):
        gate, up, down, proj, dq, dk, dv = program(
            sizes, moe_input, out_grad, routes.T, route_weight.T, w_gate[0], w_up[0], w_down[0],
            w_out, query[0], key[0], value[0], log_decay, state_in[0, 0])
        return gate[None], up[None], down[None], proj, dq[None], dk[None], dv[None]

    rows, heads = P("sp", None), P("tp", "sp", None)
    columns, lines = P("sp", None, "tp"), P("sp", "tp", None)
    return jax.shard_map(
        body,
        mesh=mesh,
        in_specs=(rows, rows, rows, rows, columns, columns, lines, P(None, "tp"),
                  heads, heads, heads, P("tp", "sp"), P("tp", "sp", None, None)),
        out_specs=(columns, columns, lines, P("sp", "tp"), heads, heads, heads),
        check_vma=False,
    )
```
